32 devices in a mesh: fs: 4 (over y, x), tp: 8 (over z, core).
Axes of the slice: x: 2, y: 2, z: 4, core: 2. Of those that a mesh axis runs over, the one named last changes fastest.
Arguments:
- normed_inputs: bfloat16 [4096, 4096], P('fs', 'tp'), may hold values from -6 to 6
- query_upstream: bfloat16 [4096, 4096], P('fs', 'tp'), may hold values from -0.125 to 0.125
- key_upstream: bfloat16 [4096, 1024], P('fs', 'tp'), may hold values from -0.09375 to 0.09375
- head_outputs: bfloat16 [4096, 4096], P('fs', 'tp'), may hold values from -6 to 6
- branch_upstream: bfloat16 [4096, 4096], P('fs', 'tp'), may hold values from -0.125 to 0.125
- query_master: float32 [4096, 4096], P('fs', 'tp'), may hold values from -0.09375 to 0.09375
- key_master: float32 [4096, 1024], P('fs', 'tp'), may hold values from -0.09375 to 0.09375
- branch_master: float32 [4096, 4096], P('fs', 'tp'), may hold values from -0.09375 to 0.09375
- query_basis: bfloat16 [4096, 128], replicated, may hold values from -0.09375 to 0.09375
- key_basis: bfloat16 [4096, 128], replicated, may hold values from -0.09375 to 0.09375
- branch_basis: bfloat16 [4096, 128], replicated, may hold values from -0.09375 to 0.09375
- query_first: float32 [128, 4096], P(None, 'tp'), may hold values from -0.75 to 0.75
- query_second: float32 [128, 4096], P(None, 'tp'), may hold values from 0.001 to 0.02
- key_first: float32 [128, 1024], P(None, 'tp'), may hold values from -0.75 to 0.75
- key_second: float32 [128, 1024], P(None, 'tp'), may hold values from 0.001 to 0.02
- branch_first: float32 [4096, 128], P('fs'), may hold values from -0.75 to 0.75
- branch_second: float32 [4096, 128], P('fs'), may hold values from 0.001 to 0.02
Outputs:
- query_step: float32 [4096, 4096], P('fs', 'tp')
- key_step: float32 [4096, 1024], P('fs', 'tp')
- branch_step: float32 [4096, 4096], P('fs', 'tp')
- query_updated: float32 [4096, 4096], P('fs', 'tp')
- key_updated: float32 [4096, 1024], P('fs', 'tp')
- branch_updated: float32 [4096, 4096], P('fs', 'tp')
- query_copy: bfloat16 [4096, 4096], P(None, 'tp')
- key_copy: bfloat16 [4096, 1024], P(None, 'tp')
- branch_copy: bfloat16 [4096, 4096], P(None, 'tp')
- query_first_new: float32 [128, 4096], P(None, 'tp')
- query_second_new: float32 [128, 4096], P(None, 'tp')
- key_first_new: float32 [128, 1024], P(None, 'tp')
- key_second_new: float32 [128, 1024], P(None, 'tp')
- branch_first_new: float32 [4096, 128], P('fs')
- branch_second_new: float32 [4096, 128], P('fs')
The draws below stay inside these ranges and needn't reach their ends.
All inputs are finite; a program needn't handle non-finite values.
Results may differ from the reference program's by a relative error of at most 0.001.
Values may be sent and summed in bfloat16 or wider, within the bound.
A program may use at most 128 MiB of HBM per device.

```python
import math
import jax
import jax.numpy as jnp
from jax import lax

D = 4096
RANK = 128
HW = 4096
KW = 1024
TOKENS = 4096


def strengthened(drawn, own_key, source, target, blocks, factor):
    def block_of(axis_at):
        return (jnp.arange(drawn.shape[axis_at]) // (drawn.shape[axis_at] // blocks)).reshape((-1,) + (1,) * (drawn.ndim - 1 - axis_at))

    near = jax.random.permutation(own_key, blocks)[block_of(target)]
    other_side = (block_of(target) + blocks // 2) % blocks
    return jnp.where((block_of(source) == near) | (block_of(source) == other_side), factor * drawn, drawn)


def steps_of(key, extent, split, least, top_value):
    def one(position, blocks):
        draws = jax.random.uniform(jax.random.fold_in(jax.random.fold_in(key, 6), position), (blocks,), jnp.float32, least / len(split), top_value / len(split))
        return jnp.repeat(jnp.exp(draws), extent[position] // blocks).reshape((-1,) + (1,) * (len(extent) - position - 1))

    loudness = one(*split[0])
    for cut in split[1:]:
        loudness = loudness * one(*cut)
    return loudness


def centred(rng, extent, width, most, cuts=(), held_as=jnp.bfloat16):
    values = width * jax.random.normal(rng, extent, jnp.float32)
    if cuts:
        values = values * steps_of(rng, extent, cuts, -0.22, 0.18)
    return jnp.clip(values, -most, most).astype(held_as)


def gaussian_with(stream_key, dims, spread, limit, shards, heavy, kind=jnp.bfloat16):
    drawn = spread * jax.random.normal(stream_key, dims, jnp.float32)
    if shards:
        drawn = drawn * steps_of(stream_key, dims, shards, -0.22, 0.18)
    return jnp.clip(strengthened(drawn, jax.random.fold_in(stream_key, 3), *heavy), -limit, limit).astype(kind)


def setup_inputs(seed: int = 0) -> dict:
    key_list = jax.random.split(jax.random.key(seed), 18)
    normed_inputs = centred(key_list[0], (TOKENS, D), 1.0, 6.0, ((0, 4), (1, 8)))
    query_upstream = gaussian_with(key_list[1], (TOKENS, HW), TOKENS ** -0.5, 0.125, ((0, 4), (1, 8)), (0, 1, 8, 2.0))
    key_upstream = centred(key_list[2], (TOKENS, KW), TOKENS ** -0.5, 0.09375, ((0, 4), (1, 8)))
    head_outputs = centred(key_list[3], (TOKENS, HW), 1.0, 6.0, ((0, 4), (1, 8)))
    branch_upstream = gaussian_with(key_list[4], (TOKENS, D), TOKENS ** -0.5, 0.125, ((0, 4), (1, 8)), (0, 1, 8, 2.0))
    query_master = centred(key_list[5], (D, HW), D ** -0.5, 0.09375, ((0, 4), (1, 8)), jnp.float32)
    key_master = centred(key_list[6], (D, KW), D ** -0.5, 0.09375, ((0, 4), (1, 8)), jnp.float32)
    branch_master = centred(key_list[7], (HW, D), HW ** -0.5, 0.09375, ((0, 4), (1, 8)), jnp.float32)
    query_basis = centred(key_list[8], (D, RANK), D ** -0.5, 0.09375)
    key_basis = centred(key_list[9], (D, RANK), D ** -0.5, 0.09375)
    branch_basis = centred(key_list[10], (D, RANK), D ** -0.5, 0.09375)
    query_first = centred(key_list[11], (RANK, HW), 0.05, 0.75, ((1, 8),), jnp.float32)
    query_second = jnp.clip(jnp.exp(math.log(0.02) - 2.9957322 * jax.random.uniform(key_list[12], (RANK, HW), jnp.float32) ** steps_of(key_list[12], (RANK, HW), ((1, 8),), -0.2, 0.2)), 0.001, 0.02)
    key_first = centred(key_list[13], (RANK, KW), 0.05, 0.75, ((1, 8),), jnp.float32)
    key_second = jnp.clip(jnp.exp(math.log(0.02) - 2.9957322 * jax.random.uniform(key_list[14], (RANK, KW), jnp.float32) ** steps_of(key_list[14], (RANK, KW), ((1, 8),), -0.2, 0.2)), 0.001, 0.02)
    branch_first = centred(key_list[15], (HW, RANK), 0.05, 0.75, ((0, 4),), jnp.float32)
    branch_second = jnp.clip(jnp.exp(math.log(0.02) - 2.9957322 * jax.random.uniform(key_list[16], (HW, RANK), jnp.float32) ** steps_of(key_list[16], (HW, RANK), ((0, 4),), -0.2, 0.2)), 0.001, 0.02)
    return {"normed_inputs": normed_inputs, "query_upstream": query_upstream, "key_upstream": key_upstream, "head_outputs": head_outputs, "branch_upstream": branch_upstream, "query_master": query_master, "key_master": key_master, "branch_master": branch_master, "query_basis": query_basis, "key_basis": key_basis, "branch_basis": branch_basis, "query_first": query_first, "query_second": query_second, "key_first": key_first, "key_second": key_second, "branch_first": branch_first, "branch_second": branch_second}


LEARN = 0.02
BETA_ONE = 0.9
BETA_TWO = 0.95
ADAM_EPS = 1e-08
CLIP_RMS = 0.5

def moments(first, second, low, clip):
    scaled = clip * low
    first_new = BETA_ONE * first + (1.0 - BETA_ONE) * scaled
    second_new = BETA_TWO * second + (1.0 - BETA_TWO) * scaled * scaled
    return (first_new, second_new, first_new / (jnp.sqrt(second_new) + ADAM_EPS))

def reference(normed_inputs, query_upstream, key_upstream, head_outputs, branch_upstream, query_master, key_master, branch_master, query_basis, key_basis, branch_basis, query_first, query_second, key_first, key_second, branch_first, branch_second):
    exact = lax.Precision.HIGHEST
    query_grad = jnp.dot(normed_inputs.T, query_upstream, preferred_element_type=jnp.float32)
    key_grad = jnp.dot(normed_inputs.T, key_upstream, preferred_element_type=jnp.float32)
    branch_grad = jnp.dot(head_outputs.T, branch_upstream, preferred_element_type=jnp.float32)
    query_low = jnp.dot(query_basis.astype(jnp.float32).T, query_grad, precision=exact)
    key_low = jnp.dot(key_basis.astype(jnp.float32).T, key_grad, precision=exact)
    branch_low = jnp.dot(branch_grad, branch_basis.astype(jnp.float32), precision=exact)
    total = jnp.sum(query_low * query_low) + jnp.sum(key_low * key_low) + jnp.sum(branch_low * branch_low)
    entries = query_low.size + key_low.size + branch_low.size
    rms_value = jnp.sqrt(total / float(entries))
    clip = 1.0 / jnp.maximum(1.0, rms_value / CLIP_RMS)
    q_first, q_second, q_dir = moments(query_first, query_second, query_low, clip)
    k_first, k_second, k_dir = moments(key_first, key_second, key_low, clip)
    b_first, b_second, b_dir = moments(branch_first, branch_second, branch_low, clip)
    query_step = jnp.dot(query_basis.astype(jnp.float32), q_dir, precision=exact)
    key_step = jnp.dot(key_basis.astype(jnp.float32), k_dir, precision=exact)
    branch_step = jnp.dot(b_dir, branch_basis.astype(jnp.float32).T, precision=exact)
    query_updated = query_master - LEARN * query_step
    key_updated = key_master - LEARN * key_step
    branch_updated = branch_master - LEARN * branch_step
    return (query_step, key_step, branch_step, query_updated, key_updated, branch_updated, query_updated.astype(jnp.bfloat16), key_updated.astype(jnp.bfloat16), branch_updated.astype(jnp.bfloat16), q_first, q_second, k_first, k_second, b_first, b_second)
```

```python
import jax
import jax.numpy as jnp
from jax import lax
from jax.sharding import PartitionSpec as P

LEARN = 0.02
BETA_ONE = 0.9
BETA_TWO = 0.95
ADAM_EPS = 1e-08
CLIP_RMS = 0.5


def moments(first, second, low, clip):
    scaled = clip * low
    first_new = BETA_ONE * first + (1.0 - BETA_ONE) * scaled
    second_new = BETA_TWO * second + (1.0 - BETA_TWO) * scaled * scaled
    return (first_new, second_new, first_new / (jnp.sqrt(second_new) + ADAM_EPS))


def over_tokens(left, right, precision=None):
    return lax.dot_general(
        left,
        right,
        (((0,), (0,)), ((), ())),
        precision=precision,
        preferred_element_type=jnp.float32,
    )


def per_device(
    normed_inputs,
    query_upstream,
    key_upstream,
    head_outputs,
    branch_upstream,
    query_master,
    key_master,
    branch_master,
    query_basis,
    key_basis,
    branch_basis,
    query_first,
    query_second,
    key_first,
    key_second,
    branch_first,
    branch_second,
):
    exact = lax.Precision.HIGHEST
    row_index = lax.axis_index("fs")
    col_index = lax.axis_index("tp")
    n_rows = lax.axis_size("fs")
    n_cols = lax.axis_size("tp")
    features = normed_inputs.shape[1]
    query_local = query_upstream.shape[1]
    key_local = key_upstream.shape[1]
    rows_in = query_master.shape[0]
    rank = query_basis.shape[1]
    def own_block(basis):
        return lax.dynamic_slice_in_dim(basis, col_index * features, features, 0)

    block_branch = own_block(branch_basis)
    proj_query, proj_key, proj_branch = lax.psum(
        (
            jnp.dot(normed_inputs, own_block(query_basis), preferred_element_type=jnp.float32),
            jnp.dot(normed_inputs, own_block(key_basis), preferred_element_type=jnp.float32),
            jnp.dot(branch_upstream, block_branch, preferred_element_type=jnp.float32),
        ),
        "tp",
    )
    part_query = over_tokens(proj_query, query_upstream.astype(jnp.float32), exact)
    part_key = over_tokens(proj_key, key_upstream.astype(jnp.float32), exact)
    part_branch = over_tokens(head_outputs.astype(jnp.float32), proj_branch, exact)
    own_branch = block_branch.astype(jnp.float32)
    query_low, key_low, branch_block = lax.psum((part_query, part_key, part_branch), "fs")
    local_squares = (
        jnp.sum(query_low * query_low)
        + jnp.sum(key_low * key_low)
        + jnp.sum(branch_block * branch_block)
    )
    rows_block = branch_block.shape[0]
    carried = jnp.concatenate([branch_block, jnp.full((8, rank), local_squares)], axis=0)
    gathered = lax.all_gather(carried, "tp", axis=0)
    total = jnp.sum(gathered[:, rows_block, 0])
    branch_all = gathered[:, :rows_block, :].reshape(n_cols * rows_block, rank)
    own_rows = branch_first.shape[0]
    branch_low = lax.dynamic_slice_in_dim(branch_all, row_index * own_rows, own_rows, 0)
    entries = rank * n_cols * (2 * query_local + key_local)
    rms_value = jnp.sqrt(total / float(entries))
    clip = 1.0 / jnp.maximum(1.0, rms_value / CLIP_RMS)
    q_first, q_second, q_dir = moments(query_first, query_second, query_low, clip)
    k_first, k_second, k_dir = moments(key_first, key_second, key_low, clip)
    b_first, b_second, b_dir = moments(branch_first, branch_second, branch_low, clip)
    step_rows_query = lax.dynamic_slice_in_dim(query_basis, row_index * rows_in, rows_in, 0).astype(
        jnp.float32
    )
    step_rows_key = lax.dynamic_slice_in_dim(key_basis, row_index * rows_in, rows_in, 0).astype(
        jnp.float32
    )
    query_step = jnp.dot(step_rows_query, q_dir, precision=exact)
    key_step = jnp.dot(step_rows_key, k_dir, precision=exact)
    branch_step = jnp.dot(b_dir, own_branch.T, precision=exact)
    query_updated = query_master - LEARN * query_step
    key_updated = key_master - LEARN * key_step
    branch_updated = branch_master - LEARN * branch_step
    query_copy, key_copy, branch_copy = (
        lax.all_gather(query_updated.astype(jnp.bfloat16), "fs", axis=0, tiled=True),
        lax.all_gather(key_updated.astype(jnp.bfloat16), "fs", axis=0, tiled=True),
        lax.all_gather(branch_updated.astype(jnp.bfloat16), "fs", axis=0, tiled=True),
    )
    return (
        query_step,
        key_step,
        branch_step,
        query_updated,
        key_updated,
        branch_updated,
        query_copy,
        key_copy,
        branch_copy,
        q_first,
        q_second,
        k_first,
        k_second,
        b_first,
        b_second,
    )


def solution(mesh):
    return jax.shard_map(
        per_device,
        mesh=mesh,
        in_specs=(
            P("fs", "tp"),
            P("fs", "tp"),
            P("fs", "tp"),
            P("fs", "tp"),
            P("fs", "tp"),
            P("fs", "tp"),
            P("fs", "tp"),
            P("fs", "tp"),
            P(),
            P(),
            P(),
            P(None, "tp"),
            P(None, "tp"),
            P(None, "tp"),
            P(None, "tp"),
            P("fs", None),
            P("fs", None),
        ),
        out_specs=(
            P("fs", "tp"),
            P("fs", "tp"),
            P("fs", "tp"),
            P("fs", "tp"),
            P("fs", "tp"),
            P("fs", "tp"),
            P(None, "tp"),
            P(None, "tp"),
            P(None, "tp"),
            P(None, "tp"),
            P(None, "tp"),
            P(None, "tp"),
            P(None, "tp"),
            P("fs", None),
            P("fs", None),
        ),
        check_vma=False,
    )
```

```python
import functools

import jax
import jax.numpy as jnp
from jax import lax
from jax.experimental import pallas as pl
from jax.experimental.pallas import tpu as pltpu
from jax.sharding import PartitionSpec as P

LEARN = 0.02
BETA_ONE = 0.9
BETA_TWO = 0.95
ADAM_EPS = 1e-08
CLIP_RMS = 0.5


def moments(first, second, low, clip):
    scaled = clip * low
    first_new = BETA_ONE * first + (1.0 - BETA_ONE) * scaled
    second_new = BETA_TWO * second + (1.0 - BETA_TWO) * scaled * scaled
    return (first_new, second_new, first_new / (jnp.sqrt(second_new) + ADAM_EPS))


def over_tokens(left, right, precision=None):
    return lax.dot_general(
        left,
        right,
        (((0,), (0,)), ((), ())),
        precision=precision,
        preferred_element_type=jnp.float32,
    )


def split_three(values):
    high = values.astype(jnp.bfloat16)
    rest = values - high.astype(jnp.float32)
    middle = rest.astype(jnp.bfloat16)
    low = (rest - middle.astype(jnp.float32)).astype(jnp.bfloat16)
    return high, middle, low


class Sender:
    def __init__(self, send_sem, recv_sem):
        self.send_sem, self.recv_sem, self.used, self.started = send_sem, recv_sem, 0, []

    def start(self, source, target, device):
        copy = pltpu.make_async_remote_copy(
            src_ref=source,
            dst_ref=target,
            send_sem=self.send_sem.at[self.used],
            recv_sem=self.recv_sem.at[self.used],
            device_id=device,
            device_id_type=pl.DeviceIdType.MESH,
        )
        self.used += 1
        copy.start()
        self.started.append(copy)
        return copy

    def drain(self):
        for copy in self.started:
            copy.wait_send()


def greet(nf, nt, row, col, both):
    barrier = pltpu.get_barrier_semaphore()
    peers = [{"fs": lax.rem(row + o, nf), "tp": col} for o in range(1, nf)]
    if both:
        peers += [{"fs": row, "tp": lax.rem(col + o, nt)} for o in range(1, nt)]
    for peer in peers:
        pl.semaphore_signal(
            barrier, inc=1, device_id=peer, device_id_type=pl.DeviceIdType.MESH
        )
    pl.semaphore_wait(barrier, len(peers))


def reduce_kernel(
    nf, nt,
    x_ref, qu_ref, ku_ref, h_ref, bu_ref, qb_ref, kb_ref, bb_ref,
    qk_out, b_out, total_out,
    part, from_pair, halves, arrived, whole, other,
    part_qk, part_b, got_qk, got_b, all_qk, all_b, spread_b, sums,
    send_sem, recv_sem,
):
    row, col = lax.axis_index("fs"), lax.axis_index("tp")
    core, height = lax.rem(col, 2), lax.div(col, 2)
    nz = nt // 2
    rank = qb_ref.shape[1]
    half = x_ref.shape[0] // 2
    piece = half // nz
    query_cols = qu_ref.shape[1]
    greet(nf, nt, row, col, True)
    sender = Sender(send_sem, recv_sem)
    pair = {"fs": row, "tp": height * 2 + (1 - core)}

    def above(o):
        return {"fs": row, "tp": lax.rem(height + o, nz) * 2 + core}

    def beside(o):
        return {"fs": lax.rem(row + o, nf), "tp": col}

    def project(which):
        rows = pl.ds(pl.multiple_of(which * half, half), half)
        x = x_ref[rows, :]
        return (
            jnp.dot(x, qb_ref[...], preferred_element_type=jnp.float32),
            jnp.dot(x, kb_ref[...], preferred_element_type=jnp.float32),
            jnp.dot(bu_ref[rows, :], bb_ref[...], preferred_element_type=jnp.float32),
        )

    for n, value in enumerate(project(1 - core)):
        part[:, n * rank : (n + 1) * rank] = value
    swap = sender.start(part, from_pair, pair)
    own = project(core)
    swap.wait_recv()
    for n, value in enumerate(own):
        span = slice(n * rank, (n + 1) * rank)
        halves[:, :, span] = (value + from_pair[:, span]).reshape(nz, piece, rank)
    copies = [
        sender.start(halves.at[lax.rem(height + o, nz)], arrived.at[o - 1], above(o))
        for o in range(1, nz)
    ]
    total = halves[height]
    for o, copy in enumerate(copies):
        copy.wait_recv()
        total = total + arrived[o]
    whole[height] = total
    copies = [sender.start(whole.at[height], whole.at[height], above(o)) for o in range(1, nz)]
    across = [sender.start(whole.at[height], other.at[height], pair)]
    for o, copy in enumerate(copies, 1):
        copy.wait_recv()
        source = lax.rem(height + nz - o, nz)
        across.append(sender.start(whole.at[source], other.at[source], pair))

    over_rows = (((0,), (0,)), ((), ()))

    def low_parts(values, which):
        rows = pl.ds(pl.multiple_of(which * half, half), half)
        sides = (qu_ref[rows, :], ku_ref[rows, :], h_ref[rows, :])
        parts = []
        for n, side in enumerate(sides):
            terms = split_three(values[:, n * rank : (n + 1) * rank])
            parts.append(
                sum(
                    lax.dot_general(term, side, over_rows, preferred_element_type=jnp.float32)
                    for term in terms
                )
            )
        return parts

    first = low_parts(whole[...].reshape(half, 3 * rank), core)
    for copy in across:
        copy.wait_recv()
    second = low_parts(other[...].reshape(half, 3 * rank), 1 - core)
    query_part, key_part, branch_part = [a + b for a, b in zip(first, second)]
    part_qk[:, :, :query_cols] = query_part.reshape(nf, rank // nf, query_cols)
    part_qk[:, :, query_cols:] = key_part.reshape(nf, rank // nf, key_part.shape[1])
    part_b[...] = branch_part.T.reshape(part_b.shape)

    copies = []
    for o in range(1, nf):
        to = lax.rem(row + o, nf)
        copies.append(sender.start(part_qk.at[to], got_qk.at[o - 1], beside(o)))
        copies.append(sender.start(part_b.at[to], got_b.at[o - 1], beside(o)))
    for copy in copies:
        copy.wait_recv()
    sum_qk, sum_b = part_qk[row], part_b[row]
    for o in range(nf - 1):
        sum_qk = sum_qk + got_qk[o]
        sum_b = sum_b + got_b[o]
    rows_b = sum_b.shape[0]
    squares = jnp.sum(sum_qk * sum_qk) + jnp.sum(sum_b * sum_b)
    all_qk[row] = sum_qk
    all_b[col, :rows_b, :] = sum_b
    all_b[col, rows_b:, :] = jnp.full((8, rank), squares, jnp.float32)

    copies_b = [
        sender.start(all_b.at[col], all_b.at[col], {"fs": row, "tp": lax.rem(col + o, nt)})
        for o in range(1, nt)
    ]
    copies_qk = [sender.start(all_qk.at[row], all_qk.at[row], beside(o)) for o in range(1, nf)]
    for copy in copies_b:
        copy.wait_recv()
    sums[row] = jnp.sum(all_b[:, rows_b:, :], axis=0)
    each = nt // nf
    copies = []
    for o in range(1, nf):
        blocks = pl.ds(lax.rem(row + o, nf) * each, each)
        copies.append(sender.start(sums.at[row], sums.at[row], beside(o)))
        copies.append(sender.start(all_b.at[blocks], spread_b.at[row], beside(o)))
    b_out[:, row] = all_b[pl.ds(row * each, each)][:, :rows_b, :]
    for copy in copies_qk:
        copy.wait_recv()
    qk_out[...] = all_qk[...].reshape(qk_out.shape)
    for copy in copies:
        copy.wait_recv()
    for o in range(1, nf):
        source = lax.rem(row + o, nf)
        b_out[:, source] = spread_b[source][:, :rows_b, :]
    total_out[...] = jnp.sum(sums[...], axis=0)
    sender.drain()


def reduced(nf, nt, x, qu, ku, h, bu, qb, kb, bb):
    tokens, features = x.shape
    rank = qb.shape[1]
    cols = qu.shape[1] + ku.shape[1]
    half, nz, each = tokens // 2, nt // 2, nt // nf
    piece, thin, rows_b = half // nz, rank // nf, features // nf
    copies = 1 + 2 * (nz - 1) + nz + 2 * (nf - 1) + (nt - 1) + 3 * (nf - 1)
    vmem = pl.BlockSpec(memory_space=pltpu.VMEM)
    f32 = jnp.float32
    return pl.pallas_call(
        functools.partial(reduce_kernel, nf, nt),
        out_shape=(
            jax.ShapeDtypeStruct((rank, cols), f32),
            jax.ShapeDtypeStruct((each, nf, rows_b, rank), f32),
            jax.ShapeDtypeStruct((8, rank), f32),
        ),
        in_specs=[vmem] * 8,
        out_specs=(vmem,) * 3,
        scratch_shapes=[
            pltpu.VMEM((half, 3 * rank), f32),
            pltpu.VMEM((half, 3 * rank), f32),
            pltpu.VMEM((nz, piece, 3 * rank), f32),
            pltpu.VMEM((nz - 1, piece, 3 * rank), f32),
            pltpu.VMEM((nz, piece, 3 * rank), f32),
            pltpu.VMEM((nz, piece, 3 * rank), f32),
            pltpu.VMEM((nf, thin, cols), f32),
            pltpu.VMEM((nf, rows_b, rank), f32),
            pltpu.VMEM((nf - 1, thin, cols), f32),
            pltpu.VMEM((nf - 1, rows_b, rank), f32),
            pltpu.VMEM((nf, thin, cols), f32),
            pltpu.VMEM((nt, rows_b + 8, rank), f32),
            pltpu.VMEM((nf, each, rows_b + 8, rank), f32),
            pltpu.VMEM((nf, 8, rank), f32),
            pltpu.SemaphoreType.DMA((copies,)),
            pltpu.SemaphoreType.DMA((copies,)),
        ],
        compiler_params=pltpu.CompilerParams(
            collective_id=0, has_side_effects=True, vmem_limit_bytes=48 * 2**20
        ),
    )(x, qu, ku, h, bu, qb, kb, bb)


def gather_kernel(nf, nt, q_ref, b_ref, k_ref, q_out, b_out, k_out, send_sem, recv_sem, own_sem):
    row, col = lax.axis_index("fs"), lax.axis_index("tp")
    greet(nf, nt, row, col, False)
    sender = Sender(send_sem, recv_sem)
    pairs = ((q_ref, q_out), (b_ref, b_out), (k_ref, k_out))
    local = []
    if nf == 4:
        side = row + 1 - 2 * lax.rem(row, 2)
        front = lax.rem(row + 2, 4)
        half = q_ref.shape[0] // 2
        names = ({"fs": side, "tp": col}, {"fs": front, "tp": col})
        forwards = []
        for ref, out in pairs:
            for h in range(2):
                rows = pl.ds(h * half, half)
                for n in ((0, 1), (1, 0))[h]:
                    copy = sender.start(ref.at[rows], out.at[row, rows], names[n])
                    forwards.append((n, h, out, copy))
        for n, (ref, out) in enumerate(pairs):
            local.append(pltpu.make_async_copy(ref, out.at[row], own_sem.at[n]))
            local[-1].start()
        last = []
        for n, h, out, copy in forwards:
            copy.wait_recv()
            if n == h:
                source = (side, front)[n]
                held = out.at[source, pl.ds(h * half, half)]
                last.append(sender.start(held, held, names[1 - n]))
        for copy in last:
            copy.wait_recv()
    else:
        copies = [
            sender.start(ref, out.at[row], {"fs": lax.rem(row + o, nf), "tp": col})
            for ref, out in pairs
            for o in range(1, nf)
        ]
        for n, (ref, out) in enumerate(pairs):
            local.append(pltpu.make_async_copy(ref, out.at[row], own_sem.at[n]))
            local[-1].start()
        for copy in copies:
            copy.wait_recv()
    for copy in local:
        copy.wait()
    sender.drain()


def gathered_rows(nf, nt, *blocks):
    count = 18 if nf == 4 else 3 * (nf - 1)
    wide = [jax.ShapeDtypeStruct((nf, *block.shape), block.dtype) for block in blocks]
    outs = pl.pallas_call(
        functools.partial(gather_kernel, nf, nt),
        out_shape=tuple(wide),
        in_specs=[pl.BlockSpec(memory_space=pltpu.VMEM)] * 3,
        out_specs=(pl.BlockSpec(memory_space=pl.ANY),) * 3,
        scratch_shapes=[
            pltpu.SemaphoreType.DMA((count,)),
            pltpu.SemaphoreType.DMA((count,)),
            pltpu.SemaphoreType.DMA((3,)),
        ],
        compiler_params=pltpu.CompilerParams(
            collective_id=1, has_side_effects=True, vmem_limit_bytes=16 * 2**20
        ),
    )(*blocks)
    return [out.reshape(-1, out.shape[-1]) for out in outs]


def per_device(
    normed_inputs,
    query_upstream,
    key_upstream,
    head_outputs,
    branch_upstream,
    query_master,
    key_master,
    branch_master,
    query_basis,
    key_basis,
    branch_basis,
    query_first,
    query_second,
    key_first,
    key_second,
    branch_first,
    branch_second,
):
    exact = lax.Precision.HIGHEST
    row_index = lax.axis_index("fs")
    col_index = lax.axis_index("tp")
    n_rows = lax.axis_size("fs")
    n_cols = lax.axis_size("tp")
    features = normed_inputs.shape[1]
    query_local = query_upstream.shape[1]
    key_local = key_upstream.shape[1]
    rows_in = query_master.shape[0]
    rank = query_basis.shape[1]
    def own_block(basis):
        return lax.dynamic_slice_in_dim(basis, col_index * features, features, 0)

    block_branch = own_block(branch_basis)
    own_branch = block_branch.astype(jnp.float32)
    lanes = -key_local % 128
    low, branch_low, squares = reduced(
        n_rows,
        n_cols,
        normed_inputs,
        query_upstream,
        jnp.pad(key_upstream, ((0, 0), (0, lanes))),
        head_outputs,
        branch_upstream,
        own_block(query_basis),
        own_block(key_basis),
        block_branch,
    )
    query_low = low[:, :query_local]
    key_low = low[:, query_local : query_local + key_local]
    branch_low = branch_low.reshape(branch_first.shape)
    total = squares[0, 0]
    entries = rank * n_cols * (2 * query_local + key_local)
    rms_value = jnp.sqrt(total / float(entries))
    clip = 1.0 / jnp.maximum(1.0, rms_value / CLIP_RMS)
    q_first, q_second, q_dir = moments(query_first, query_second, query_low, clip)
    k_first, k_second, k_dir = moments(key_first, key_second, key_low, clip)
    b_first, b_second, b_dir = moments(branch_first, branch_second, branch_low, clip)
    step_rows_query = lax.dynamic_slice_in_dim(query_basis, row_index * rows_in, rows_in, 0).astype(
        jnp.float32
    )
    step_rows_key = lax.dynamic_slice_in_dim(key_basis, row_index * rows_in, rows_in, 0).astype(
        jnp.float32
    )
    query_step = jnp.dot(step_rows_query, q_dir, precision=exact)
    key_step = jnp.dot(step_rows_key, k_dir, precision=exact)
    branch_step = jnp.dot(b_dir, own_branch.T, precision=exact)
    query_updated = query_master - LEARN * query_step
    key_updated = key_master - LEARN * key_step
    branch_updated = branch_master - LEARN * branch_step
    query_copy, branch_copy, key_copy = gathered_rows(
        n_rows,
        n_cols,
        query_updated.astype(jnp.bfloat16),
        branch_updated.astype(jnp.bfloat16),
        jnp.pad(key_updated, ((0, 0), (0, lanes))).astype(jnp.bfloat16),
    )
    key_copy = key_copy[:, :key_local]
    return (
        query_step,
        key_step,
        branch_step,
        query_updated,
        key_updated,
        branch_updated,
        query_copy,
        key_copy,
        branch_copy,
        q_first,
        q_second,
        k_first,
        k_second,
        b_first,
        b_second,
    )


def solution(mesh):
    return jax.shard_map(
        per_device,
        mesh=mesh,
        in_specs=(
            P("fs", "tp"),
            P("fs", "tp"),
            P("fs", "tp"),
            P("fs", "tp"),
            P("fs", "tp"),
            P("fs", "tp"),
            P("fs", "tp"),
            P("fs", "tp"),
            P(),
            P(),
            P(),
            P(None, "tp"),
            P(None, "tp"),
            P(None, "tp"),
            P(None, "tp"),
            P("fs", None),
            P("fs", None),
        ),
        out_specs=(
            P("fs", "tp"),
            P("fs", "tp"),
            P("fs", "tp"),
            P("fs", "tp"),
            P("fs", "tp"),
            P("fs", "tp"),
            P(None, "tp"),
            P(None, "tp"),
            P(None, "tp"),
            P(None, "tp"),
            P(None, "tp"),
            P(None, "tp"),
            P(None, "tp"),
            P("fs", None),
            P("fs", None),
        ),
        check_vma=False,
    )
```

```python
import functools

import jax
import jax.numpy as jnp
from jax import lax
from jax.experimental import pallas as pl
from jax.experimental.pallas import tpu as pltpu
from jax.sharding import PartitionSpec as P

LEARN = 0.02
BETA_ONE = 0.9
BETA_TWO = 0.95
ADAM_EPS = 1e-08
CLIP_RMS = 0.5


def moments(first, second, low, clip):
    scaled = clip * low
    first_new = BETA_ONE * first + (1.0 - BETA_ONE) * scaled
    second_new = BETA_TWO * second + (1.0 - BETA_TWO) * scaled * scaled
    return (first_new, second_new, first_new / (jnp.sqrt(second_new) + ADAM_EPS))


def over_tokens(left, right, precision=None):
    return lax.dot_general(
        left,
        right,
        (((0,), (0,)), ((), ())),
        precision=precision,
        preferred_element_type=jnp.float32,
    )


def split_three(values):
    high = values.astype(jnp.bfloat16)
    rest = values - high.astype(jnp.float32)
    middle = rest.astype(jnp.bfloat16)
    low = (rest - middle.astype(jnp.float32)).astype(jnp.bfloat16)
    return high, middle, low


class Sender:
    def __init__(self, send_sem, recv_sem):
        self.send_sem, self.recv_sem, self.used, self.started = send_sem, recv_sem, 0, []

    def start(self, source, target, device):
        copy = pltpu.make_async_remote_copy(
            src_ref=source,
            dst_ref=target,
            send_sem=self.send_sem.at[self.used],
            recv_sem=self.recv_sem.at[self.used],
            device_id=device,
            device_id_type=pl.DeviceIdType.MESH,
        )
        self.used += 1
        copy.start()
        self.started.append(copy)
        return copy

    def drain(self):
        for copy in self.started:
            copy.wait_send()


def greet(nf, nt, row, col, both):
    barrier = pltpu.get_barrier_semaphore()
    peers = [{"fs": lax.rem(row + o, nf), "tp": col} for o in range(1, nf)]
    if both:
        peers += [{"fs": row, "tp": lax.rem(col + o, nt)} for o in range(1, nt)]
    for peer in peers:
        pl.semaphore_signal(
            barrier, inc=1, device_id=peer, device_id_type=pl.DeviceIdType.MESH
        )
    pl.semaphore_wait(barrier, len(peers))


def square(row, col):
    side = row + 1 - 2 * lax.rem(row, 2)
    front = lax.rem(row + 2, 4)
    return side, front, ({"fs": side, "tp": col}, {"fs": front, "tp": col})


def reduce_kernel(
    nf, nt,
    x_hbm, qu_hbm, ku_hbm, h_hbm, bu_hbm, master_ref, qb_ref, kb_ref, bb_ref,
    qk_out, b_out, total_out, far_out,
    x_ref, qu_ref, ku_ref, h_ref, bu_ref,
    part, from_pair, halves, arrived, whole, other,
    part_qk, part_b, got_qk, got_b, all_qk, all_b, spread_b, sums,
    send_sem, recv_sem, load_sem,
):
    row, col = lax.axis_index("fs"), lax.axis_index("tp")
    core, height = lax.rem(col, 2), lax.div(col, 2)
    nz = nt // 2
    rank = qb_ref.shape[1]
    half = x_ref.shape[0] // 2
    piece = half // nz
    query_cols = qu_ref.shape[1]
    loads = []

    def load(source, target):
        copy = pltpu.make_async_copy(source, target, load_sem.at[len(loads)])
        copy.start()
        loads.append(copy)

    for which in (1 - core, core):
        rows = pl.ds(pl.multiple_of(which * half, half), half)
        load(x_hbm.at[rows], x_ref.at[rows])
        load(bu_hbm.at[rows], bu_ref.at[rows])
    load(qu_hbm, qu_ref)
    load(ku_hbm, ku_ref)
    load(h_hbm, h_ref)
    greet(nf, nt, row, col, True)
    sender = Sender(send_sem, recv_sem)
    pair = {"fs": row, "tp": height * 2 + (1 - core)}

    def above(o):
        return {"fs": row, "tp": lax.rem(height + o, nz) * 2 + core}

    def beside(o):
        return {"fs": lax.rem(row + o, nf), "tp": col}

    def project(which):
        rows = pl.ds(pl.multiple_of(which * half, half), half)
        x = x_ref[rows, :]
        return (
            jnp.dot(x, qb_ref[...], preferred_element_type=jnp.float32),
            jnp.dot(x, kb_ref[...], preferred_element_type=jnp.float32),
            jnp.dot(bu_ref[rows, :], bb_ref[...], preferred_element_type=jnp.float32),
        )

    early = far_out.shape[1]
    sent = []
    if nf == 4:
        side, front, names = square(row, col)
        for turn in range(2):
            for n in range(2):
                rows = pl.ds((turn ^ n) * (early // 2), early // 2)
                sent.append(
                    sender.start(master_ref.at[rows], far_out.at[row, rows], names[n])
                )
    else:
        rows = pl.ds(0, early)
        for o in range(1, nf):
            sent.append(sender.start(master_ref.at[rows], far_out.at[row], beside(o)))
    loads[0].wait()
    loads[1].wait()
    for n, value in enumerate(project(1 - core)):
        part[:, n * rank : (n + 1) * rank] = value
    swap = sender.start(part, from_pair, pair)
    loads[2].wait()
    loads[3].wait()
    own = project(core)
    swap.wait_recv()
    for n, value in enumerate(own):
        span = slice(n * rank, (n + 1) * rank)
        halves[:, :, span] = (value + from_pair[:, span]).reshape(nz, piece, rank)
    copies = [
        sender.start(halves.at[lax.rem(height + o, nz)], arrived.at[o - 1], above(o))
        for o in range(1, nz)
    ]
    total = halves[height]
    for o, copy in enumerate(copies):
        copy.wait_recv()
        total = total + arrived[o]
    whole[height] = total
    copies = [sender.start(whole.at[height], whole.at[height], above(o)) for o in range(1, nz)]
    across = [sender.start(whole.at[height], other.at[height], pair)]
    passed = []
    if nf == 4:
        for n, source in ((0, side), (1, front)):
            sent[n].wait_recv()
            held = far_out.at[source, pl.ds(n * (early // 2), early // 2)]
            passed.append(sender.start(held, held, names[1 - n]))
    for o, copy in enumerate(copies, 1):
        copy.wait_recv()
        source = lax.rem(height + nz - o, nz)
        across.append(sender.start(whole.at[source], other.at[source], pair))

    over_rows = (((0,), (0,)), ((), ()))

    def low_parts(values, which):
        rows = pl.ds(pl.multiple_of(which * half, half), half)
        sides = (qu_ref[rows, :], ku_ref[rows, :], h_ref[rows, :])
        parts = []
        for n, side in enumerate(sides):
            terms = split_three(values[:, n * rank : (n + 1) * rank])
            parts.append(
                sum(
                    lax.dot_general(term, side, over_rows, preferred_element_type=jnp.float32)
                    for term in terms
                )
            )
        return parts

    for copy in loads[4:]:
        copy.wait()
    first = low_parts(whole[...].reshape(half, 3 * rank), core)
    for copy in across:
        copy.wait_recv()
    second = low_parts(other[...].reshape(half, 3 * rank), 1 - core)
    query_part, key_part, branch_part = [a + b for a, b in zip(first, second)]
    part_qk[:, :, :query_cols] = query_part.reshape(nf, rank // nf, query_cols)
    part_qk[:, :, query_cols:] = key_part.reshape(nf, rank // nf, key_part.shape[1])
    part_b[...] = branch_part.T.reshape(part_b.shape)

    copies = []
    for o in range(1, nf):
        to = lax.rem(row + o, nf)
        copies.append(sender.start(part_qk.at[to], got_qk.at[o - 1], beside(o)))
        copies.append(sender.start(part_b.at[to], got_b.at[o - 1], beside(o)))
    for copy in copies:
        copy.wait_recv()
    sum_qk, sum_b = part_qk[row], part_b[row]
    for o in range(nf - 1):
        sum_qk = sum_qk + got_qk[o]
        sum_b = sum_b + got_b[o]
    rows_b = sum_b.shape[0]
    squares = jnp.sum(sum_qk * sum_qk) + jnp.sum(sum_b * sum_b)
    all_qk[row] = sum_qk
    all_b[col, :rows_b, :] = sum_b
    all_b[col, rows_b:, :] = jnp.full((8, rank), squares, jnp.float32)

    copies_b = [
        sender.start(all_b.at[col], all_b.at[col], {"fs": row, "tp": lax.rem(col + o, nt)})
        for o in range(1, nt)
    ]
    copies_qk = [sender.start(all_qk.at[row], all_qk.at[row], beside(o)) for o in range(1, nf)]
    for copy in copies_b:
        copy.wait_recv()
    sums[row] = jnp.sum(all_b[:, rows_b:, :], axis=0)
    each = nt // nf
    copies = []
    for o in range(1, nf):
        blocks = pl.ds(lax.rem(row + o, nf) * each, each)
        copies.append(sender.start(sums.at[row], sums.at[row], beside(o)))
        copies.append(sender.start(all_b.at[blocks], spread_b.at[row], beside(o)))
    b_out[:, row] = all_b[pl.ds(row * each, each)][:, :rows_b, :]
    for copy in copies_qk:
        copy.wait_recv()
    qk_out[...] = all_qk[...].reshape(qk_out.shape)
    for copy in copies:
        copy.wait_recv()
    for o in range(1, nf):
        source = lax.rem(row + o, nf)
        b_out[:, source] = spread_b[source][:, :rows_b, :]
    total_out[...] = jnp.sum(sums[...], axis=0)
    for copy in (sent[2:] + passed) if nf == 4 else sent:
        copy.wait_recv()
    sender.drain()


def reduced(nf, nt, early, x, qu, ku, h, bu, master, qb, kb, bb):
    tokens, features = x.shape
    rank = qb.shape[1]
    cols = qu.shape[1] + ku.shape[1]
    half, nz, each = tokens // 2, nt // 2, nt // nf
    piece, thin, rows_b = half // nz, rank // nf, features // nf
    copies = 1 + 2 * (nz - 1) + nz + 2 * (nf - 1) + (nt - 1) + 3 * (nf - 1)
    copies += 6 if nf == 4 else nf - 1
    any_place = pl.BlockSpec(memory_space=pl.ANY)
    vmem = pl.BlockSpec(memory_space=pltpu.VMEM)
    f32 = jnp.float32
    return pl.pallas_call(
        functools.partial(reduce_kernel, nf, nt),
        out_shape=(
            jax.ShapeDtypeStruct((rank, cols), f32),
            jax.ShapeDtypeStruct((each, nf, rows_b, rank), f32),
            jax.ShapeDtypeStruct((8, rank), f32),
            jax.ShapeDtypeStruct((nf, early, master.shape[1]), f32),
        ),
        in_specs=[any_place] * 6 + [vmem] * 3,
        out_specs=(vmem, vmem, vmem, any_place),
        scratch_shapes=[
            *[pltpu.VMEM(each_in.shape, each_in.dtype) for each_in in (x, qu, ku, h, bu)],
            pltpu.VMEM((half, 3 * rank), f32),
            pltpu.VMEM((half, 3 * rank), f32),
            pltpu.VMEM((nz, piece, 3 * rank), f32),
            pltpu.VMEM((nz - 1, piece, 3 * rank), f32),
            pltpu.VMEM((nz, piece, 3 * rank), f32),
            pltpu.VMEM((nz, piece, 3 * rank), f32),
            pltpu.VMEM((nf, thin, cols), f32),
            pltpu.VMEM((nf, rows_b, rank), f32),
            pltpu.VMEM((nf - 1, thin, cols), f32),
            pltpu.VMEM((nf - 1, rows_b, rank), f32),
            pltpu.VMEM((nf, thin, cols), f32),
            pltpu.VMEM((nt, rows_b + 8, rank), f32),
            pltpu.VMEM((nf, each, rows_b + 8, rank), f32),
            pltpu.VMEM((nf, 8, rank), f32),
            pltpu.SemaphoreType.DMA((copies,)),
            pltpu.SemaphoreType.DMA((copies,)),
            pltpu.SemaphoreType.DMA((7,)),
        ],
        compiler_params=pltpu.CompilerParams(
            collective_id=0, has_side_effects=True, vmem_limit_bytes=58 * 2**20
        ),
    )(x, qu, ku, h, bu, master, qb, kb, bb)


def gather_kernel(
    nf, nt,
    q_ref, b_ref, k_ref, far_ref, master_ref, basis_ref, dir_ref,
    q_out, b_out, k_out,
    held_far, held_copy, send_sem, recv_sem, own_sem, load_sem, store_sem,
):
    row, col = lax.axis_index("fs"), lax.axis_index("tp")
    early = far_ref.shape[1]
    pairs = ((q_ref, q_out, early), (b_ref, b_out, 0), (k_ref, k_out, 0))

    def load(o):
        source = master_ref.at[pl.ds(0, early)] if o == 0 else far_ref.at[lax.rem(row + o, nf)]
        copy = pltpu.make_async_copy(source, held_far.at[o % 2], load_sem.at[o])
        copy.start()
        return copy

    coming = load(0)
    greet(nf, nt, row, col, False)
    sender = Sender(send_sem, recv_sem)
    sent = []
    if nf == 4:
        side, front, names = square(row, col)
        for ref, out, base in pairs:
            half = ref.shape[0] // 2
            for h in range(2):
                rows = pl.ds(h * half, half)
                target = pl.ds(base + h * half, half)
                for n in ((0, 1), (1, 0))[h]:
                    copy = sender.start(ref.at[rows], out.at[row, target], names[n])
                    sent.append((n, h, out, target, copy))
    else:
        for ref, out, base in pairs:
            for o in range(1, nf):
                target = out.at[row, pl.ds(base, ref.shape[0])]
                there = {"fs": lax.rem(row + o, nf), "tp": col}
                sent.append(sender.start(ref, target, there))
    local = []
    for n, (ref, out, base) in enumerate(pairs):
        target = out.at[row, pl.ds(base, ref.shape[0])]
        local.append(pltpu.make_async_copy(ref, target, own_sem.at[n]))
        local[-1].start()

    terms = split_three(dir_ref[...])
    rows_all = q_out.shape[1]
    stores = []
    for o in range(nf):
        source = lax.rem(row + o, nf)
        coming.wait()
        if o + 1 < nf:
            coming = load(o + 1)
        if o >= 2:
            stores[o - 2].wait()
        basis = basis_ref[pl.ds(pl.multiple_of(source * rows_all, rows_all), early), :]
        step = sum(jnp.dot(basis, term, preferred_element_type=jnp.float32) for term in terms)
        held_copy[o % 2] = (held_far[o % 2] - LEARN * step).astype(held_copy.dtype)
        stores.append(
            pltpu.make_async_copy(
                held_copy.at[o % 2], q_out.at[source, pl.ds(0, early)], store_sem.at[o]
            )
        )
        stores[-1].start()

    if nf == 4:
        last = []
        for n, h, out, target, copy in sent:
            copy.wait_recv()
            if n == h:
                held = out.at[(side, front)[n], target]
                last.append(sender.start(held, held, names[1 - n]))
        sent = last
    for copy in sent:
        copy.wait_recv()
    for copy in local + stores[-2:]:
        copy.wait()
    sender.drain()


def gathered_rows(nf, nt, q_tail, b_block, k_block, far, master, basis, direction):
    count = 18 if nf == 4 else 3 * (nf - 1)
    early = far.shape[1]
    blocks = (master, b_block, k_block)
    wide = [jax.ShapeDtypeStruct((nf, *block.shape), q_tail.dtype) for block in blocks]
    vmem = pl.BlockSpec(memory_space=pltpu.VMEM)
    any_place = pl.BlockSpec(memory_space=pl.ANY)
    outs = pl.pallas_call(
        functools.partial(gather_kernel, nf, nt),
        out_shape=tuple(wide),
        in_specs=[vmem] * 3 + [any_place] * 2 + [vmem] * 2,
        out_specs=(any_place,) * 3,
        scratch_shapes=[
            pltpu.VMEM((2, early, far.shape[2]), far.dtype),
            pltpu.VMEM((2, early, far.shape[2]), q_tail.dtype),
            pltpu.SemaphoreType.DMA((count,)),
            pltpu.SemaphoreType.DMA((count,)),
            pltpu.SemaphoreType.DMA((3,)),
            pltpu.SemaphoreType.DMA((nf,)),
            pltpu.SemaphoreType.DMA((nf,)),
        ],
        compiler_params=pltpu.CompilerParams(
            collective_id=1, has_side_effects=True, vmem_limit_bytes=48 * 2**20
        ),
    )(q_tail, b_block, k_block, far, master, basis, direction)
    return [out.reshape(-1, out.shape[-1]) for out in outs]


def per_device(
    normed_inputs,
    query_upstream,
    key_upstream,
    head_outputs,
    branch_upstream,
    query_master,
    key_master,
    branch_master,
    query_basis,
    key_basis,
    branch_basis,
    query_first,
    query_second,
    key_first,
    key_second,
    branch_first,
    branch_second,
):
    exact = lax.Precision.HIGHEST
    row_index = lax.axis_index("fs")
    col_index = lax.axis_index("tp")
    n_rows = lax.axis_size("fs")
    n_cols = lax.axis_size("tp")
    features = normed_inputs.shape[1]
    query_local = query_upstream.shape[1]
    key_local = key_upstream.shape[1]
    rows_in = query_master.shape[0]
    rank = query_basis.shape[1]
    def own_block(basis):
        return lax.dynamic_slice_in_dim(basis, col_index * features, features, 0)

    block_branch = own_block(branch_basis)
    own_branch = block_branch.astype(jnp.float32)
    lanes = -key_local % 128
    early = rows_in // 32 * 20
    low, branch_low, squares, far = reduced(
        n_rows,
        n_cols,
        early,
        normed_inputs,
        query_upstream,
        jnp.pad(key_upstream, ((0, 0), (0, lanes))),
        head_outputs,
        branch_upstream,
        query_master,
        own_block(query_basis),
        own_block(key_basis),
        block_branch,
    )
    query_low = low[:, :query_local]
    key_low = low[:, query_local : query_local + key_local]
    branch_low = branch_low.reshape(branch_first.shape)
    total = squares[0, 0]
    entries = rank * n_cols * (2 * query_local + key_local)
    rms_value = jnp.sqrt(total / float(entries))
    clip = 1.0 / jnp.maximum(1.0, rms_value / CLIP_RMS)
    q_first, q_second, q_dir = moments(query_first, query_second, query_low, clip)
    k_first, k_second, k_dir = moments(key_first, key_second, key_low, clip)
    b_first, b_second, b_dir = moments(branch_first, branch_second, branch_low, clip)
    step_rows_query = lax.dynamic_slice_in_dim(query_basis, row_index * rows_in, rows_in, 0).astype(
        jnp.float32
    )
    step_rows_key = lax.dynamic_slice_in_dim(key_basis, row_index * rows_in, rows_in, 0).astype(
        jnp.float32
    )
    query_step = jnp.dot(step_rows_query, q_dir, precision=exact)
    key_step = jnp.dot(step_rows_key, k_dir, precision=exact)
    branch_step = jnp.dot(b_dir, own_branch.T, precision=exact)
    query_updated = query_master - LEARN * query_step
    key_updated = key_master - LEARN * key_step
    branch_updated = branch_master - LEARN * branch_step
    query_copy, branch_copy, key_copy = gathered_rows(
        n_rows,
        n_cols,
        query_updated[early:].astype(jnp.bfloat16),
        branch_updated.astype(jnp.bfloat16),
        jnp.pad(key_updated, ((0, 0), (0, lanes))).astype(jnp.bfloat16),
        far,
        query_master,
        query_basis,
        q_dir,
    )
    key_copy = key_copy[:, :key_local]
    return (
        query_step,
        key_step,
        branch_step,
        query_updated,
        key_updated,
        branch_updated,
        query_copy,
        key_copy,
        branch_copy,
        q_first,
        q_second,
        k_first,
        k_second,
        b_first,
        b_second,
    )


def solution(mesh):
    return jax.shard_map(
        per_device,
        mesh=mesh,
        in_specs=(
            P("fs", "tp"),
            P("fs", "tp"),
            P("fs", "tp"),
            P("fs", "tp"),
            P("fs", "tp"),
            P("fs", "tp"),
            P("fs", "tp"),
            P("fs", "tp"),
            P(),
            P(),
            P(),
            P(None, "tp"),
            P(None, "tp"),
            P(None, "tp"),
            P(None, "tp"),
            P("fs", None),
            P("fs", None),
        ),
        out_specs=(
            P("fs", "tp"),
            P("fs", "tp"),
            P("fs", "tp"),
            P("fs", "tp"),
            P("fs", "tp"),
            P("fs", "tp"),
            P(None, "tp"),
            P(None, "tp"),
            P(None, "tp"),
            P(None, "tp"),
            P(None, "tp"),
            P(None, "tp"),
            P(None, "tp"),
            P("fs", None),
            P("fs", None),
        ),
        check_vma=False,
    )
```
